32 devices in a mesh: ep: 16 (over z, y, x), tp: 2 (over core).
Axes of the slice: x: 2, y: 2, z: 4, core: 2. Of those that a mesh axis runs over, the one named last changes fastest.
Arguments:
- hidden: bfloat16 [352, 2048], P('ep'), may hold values from -6 to 6
- mixer_gain: bfloat16 [2048], replicated, may hold values from 0.099609375 to 1.8984375
- gate_proj: bfloat16 [2048, 1024], P(None, 'tp'), may hold values from -0.125 to 0.125
- value_proj: bfloat16 [2048, 1024], P(None, 'tp'), may hold values from -0.125 to 0.125
- write_proj: bfloat16 [2048, 512], P(None, 'tp'), may hold values from -0.125 to 0.125
- read_proj: bfloat16 [2048, 512], P(None, 'tp'), may hold values from -0.125 to 0.125
- step_proj: bfloat16 [2048, 16], replicated, may hold values from -0.125 to 0.125
- step_bias: float32 [16], replicated, may hold values from -3 to 0
- decay_log: float32 [16], replicated, may hold values from 0 to 2.77
- skip_gain: float32 [16], replicated, may hold values from 0.5 to 2
- value_taps: bfloat16 [4, 1024], replicated, may hold values from -3 to 3
- write_taps: bfloat16 [4, 512], replicated, may hold values from -3 to 3
- read_taps: bfloat16 [4, 512], replicated, may hold values from -3 to 3
- value_tail: bfloat16 [352, 3, 1024], P('ep', None, 'tp'), may hold values from -6 to 6
- write_tail: bfloat16 [352, 3, 512], P('ep', None, 'tp'), may hold values from -6 to 6
- read_tail: bfloat16 [352, 3, 512], P('ep', None, 'tp'), may hold values from -6 to 6
- scan_state: float32 [352, 16, 64, 128], P('ep', 'tp'), may hold values from -4 to 4
- group_gain: bfloat16 [1024], replicated, may hold values from 0.099609375 to 1.8984375
- out_proj: bfloat16 [1024, 2048], P('tp'), may hold values from -0.1875 to 0.1875
- ffn_gain: bfloat16 [2048], replicated, may hold values from 0.099609375 to 1.8984375
- group_router: bfloat16 [2048, 2], replicated, may hold values from -0.125 to 0.125
- expert_router: bfloat16 [2048, 16], replicated, may hold values from -0.125 to 0.125
- expert_choice: int32 [352, 3], P('ep'), may hold values from 0 to 15, as said below
- expert_gate: bfloat16 [16, 2048, 1024], P('ep', None, 'tp'), may hold values from -0.125 to 0.125
- expert_up: bfloat16 [16, 2048, 1024], P('ep', None, 'tp'), may hold values from -0.125 to 0.125
- expert_down: bfloat16 [16, 1024, 2048], P('ep', 'tp'), may hold values from -1 to 1
Outputs:
- layer_out: bfloat16 [352, 2048], P('ep', 'tp')
- new_state: float32 [352, 16, 64, 128], P('ep', 'tp')
The draws below stay inside these ranges and needn't reach their ends.
Inputs may be any that keep to these rules, and one draw needn't show every extreme that they name: `expert_choice`: every row names 3 different experts of one group (numbers equal in // 8). The 22 rows of one device name no expert more than 6 times, and for every device some expert is named exactly 6 times.
All inputs are finite; a program needn't handle non-finite values.
Results may differ from the reference program's by a relative error of at most 0.017.
Values may be sent and summed in bfloat16 or wider, within the bound.
A program may use at most 128 MiB of HBM per device.

```python
import jax
import jax.numpy as jnp
from jax import lax

D = 2048
HEADS = 16
HEAD_DIM = 64
DI = 1024
BC_GROUPS = 4
STATE_N = 128
TAPS = 4
GROUP_SIZE = 8
TOPK = 3
EXPERT_WIDTH = 1024
SEQ_DEV = 22
TOKENS = 352
EXPERTS = 16
EXPERT_GROUPS = 2
ROUNDS = 2
CAP = 6
N_EP = 16
N_TP = 2


def draw_expert_choice(key, part):
    level = jax.random.randint(jax.random.fold_in(key, 1), (EXPERTS,), 0, 4)
    order_key = jax.random.fold_in(key, 2)
    orders = jax.vmap(lambda number: jax.random.permutation(jax.random.fold_in(order_key, number), GROUP_SIZE))(jnp.arange(EXPERT_GROUPS))
    remaining = SEQ_DEV - (ROUNDS - 1) * EXPERTS
    block_key = jax.random.fold_in(key, 3)

    def one_block(number):
        own_key = jax.random.fold_in(block_key, number)
        pieces = [jax.random.permutation(jax.random.fold_in(own_key, 10 + turn), EXPERTS) for turn in range(ROUNDS - 1)]
        noise = jax.random.randint(jax.random.fold_in(own_key, 1), (EXPERTS,), 0, 4)
        tiebreak = jax.random.permutation(jax.random.fold_in(own_key, 2), EXPERTS)
        first = jax.random.randint(jax.random.fold_in(own_key, 3), (), 0, EXPERTS)
        spots = jnp.arange(EXPERTS)
        forced = (spots // GROUP_SIZE == first // GROUP_SIZE) & ((spots - first) % GROUP_SIZE < TOPK)
        score = forced.astype(jnp.int32) * (8 * EXPERTS) + (level + noise) * EXPERTS + tiebreak
        picked = lax.top_k(score, remaining)[1]
        slots = jnp.concatenate(pieces + [picked]).astype(jnp.int32)
        shuffle = jax.random.permutation(jax.random.fold_in(own_key, 4), SEQ_DEV)
        return slots[shuffle]
    starts = jax.vmap(one_block)(jnp.arange(TOKENS // SEQ_DEV)).reshape(TOKENS)
    group = starts // GROUP_SIZE
    within = (starts % GROUP_SIZE)[:, None] + jnp.arange(TOPK)[None, :]
    chosen = group[:, None] * GROUP_SIZE + orders[group[:, None], within % GROUP_SIZE]
    return chosen.astype(jnp.int32)


def block_scale(key, extent, cuts, smallest, top_value):
    factor_of = 1.0
    for position, parts in cuts:
        steps = jax.random.uniform(jax.random.fold_in(jax.random.fold_in(key, 6), position), (parts,), jnp.float32, smallest / len(cuts), top_value / len(cuts))
        factor_of = factor_of * jnp.repeat(jnp.exp(steps), extent[position] // parts).reshape((-1,) + (1,) * (len(extent) - 1 - position))
    return factor_of


def bell_draw(key, extent, spread, limit, cuts=(), held_as=jnp.bfloat16):
    array = jax.random.normal(key, extent, jnp.float32) * spread
    if len(cuts) > 0:
        array = block_scale(key, extent, cuts, -0.22, 0.18) * array
    return jnp.clip(array, min=-limit, max=limit).astype(held_as)


def setup_inputs(seed: int = 0) -> dict:
    key_of = jax.random.split(jax.random.key(seed), 27)
    return {
        "hidden": bell_draw(key_of[0], (TOKENS, D), 1.0, 6.0, ((0, 16),)),
        "mixer_gain": jnp.clip(1.0 + 0.18 * jax.random.normal(key_of[1], (D,), jnp.float32), 0.099609375, 1.8984375).astype(jnp.bfloat16),
        "gate_proj": bell_draw(key_of[2], (D, DI), D ** -0.5, 0.125, ((1, 2),)),
        "value_proj": bell_draw(key_of[3], (D, DI), D ** -0.5, 0.125, ((1, 2),)),
        "write_proj": bell_draw(key_of[4], (D, BC_GROUPS * STATE_N), D ** -0.5, 0.125, ((1, 2),)),
        "read_proj": bell_draw(key_of[5], (D, BC_GROUPS * STATE_N), D ** -0.5, 0.125, ((1, 2),)),
        "step_proj": bell_draw(key_of[6], (D, HEADS), D ** -0.5, 0.125),
        "step_bias": jnp.clip(jax.random.uniform(key_of[7], (HEADS,), jnp.float32, -3.0, 0.0), -3.0, 0.0),
        "decay_log": jnp.clip(jax.random.uniform(key_of[8], (HEADS,), jnp.float32, 0.0, 2.77), 0.0, 2.77),
        "skip_gain": jnp.clip(jax.random.uniform(key_of[9], (HEADS,), jnp.float32, 0.5, 2.0), 0.5, 2.0),
        "value_taps": bell_draw(key_of[10], (TAPS, DI), TAPS ** -0.5, 3.0),
        "write_taps": bell_draw(key_of[11], (TAPS, BC_GROUPS * STATE_N), TAPS ** -0.5, 3.0),
        "read_taps": bell_draw(key_of[12], (TAPS, BC_GROUPS * STATE_N), TAPS ** -0.5, 3.0),
        "value_tail": bell_draw(key_of[13], (TOKENS, TAPS - 1, DI), 1.0, 6.0, ((0, 16), (2, 2))),
        "write_tail": bell_draw(key_of[14], (TOKENS, TAPS - 1, BC_GROUPS * STATE_N), 1.0, 6.0, ((0, 16), (2, 2))),
        "read_tail": bell_draw(key_of[15], (TOKENS, TAPS - 1, BC_GROUPS * STATE_N), 1.0, 6.0, ((0, 16), (2, 2))),
        "scan_state": bell_draw(key_of[16], (TOKENS, HEADS, HEAD_DIM, STATE_N), 0.3, 4.0, ((0, 16), (1, 2)), jnp.float32),
        "group_gain": jnp.clip(1.0 + 0.18 * jax.random.normal(key_of[17], (DI,), jnp.float32), 0.099609375, 1.8984375).astype(jnp.bfloat16),
        "out_proj": bell_draw(key_of[18], (DI, D), DI ** -0.5, 0.1875, ((0, 2),)),
        "ffn_gain": jnp.clip(1.0 + 0.18 * jax.random.normal(key_of[19], (D,), jnp.float32), 0.099609375, 1.8984375).astype(jnp.bfloat16),
        "group_router": bell_draw(key_of[20], (D, EXPERT_GROUPS), D ** -0.5, 0.125),
        "expert_router": bell_draw(key_of[21], (D, EXPERTS), D ** -0.5, 0.125),
        "expert_choice": draw_expert_choice(jax.random.fold_in(key_of[26], 71), 0),
        "expert_gate": bell_draw(key_of[23], (EXPERTS, D, EXPERT_WIDTH), D ** -0.5, 0.125, ((0, 16), (2, 2))),
        "expert_up": bell_draw(key_of[24], (EXPERTS, D, EXPERT_WIDTH), D ** -0.5, 0.125, ((0, 16), (2, 2))),
        "expert_down": bell_draw(key_of[25], (EXPERTS, EXPERT_WIDTH, D), (EXPERT_WIDTH // 32) ** -0.5, 1.0, ((0, 16), (1, 2))),
    }


EPSILON = 1e-06

def normed(values, gain):
    widened = values.astype(jnp.float32)
    scale = lax.rsqrt(lax.optimization_barrier(jnp.mean(widened * widened, axis=-1, keepdims=True)) + EPSILON)
    return widened * scale * gain.astype(jnp.float32)

def convolve(history, newest, kernel):
    summed = kernel[-1].astype(jnp.float32) * newest.astype(jnp.float32)
    for offset in range(history.shape[1]):
        summed = summed + kernel[offset].astype(jnp.float32) * history[:, offset].astype(jnp.float32)
    return jax.nn.silu(summed)

def project(left, right):
    return jnp.dot(left, right, preferred_element_type=jnp.float32)

def reference(hidden, mixer_gain, gate_proj, value_proj, write_proj, read_proj, step_proj, step_bias, decay_log, skip_gain, value_taps, write_taps, read_taps, value_tail, write_tail, read_tail, scan_state, group_gain, out_proj, ffn_gain, group_router, expert_router, expert_choice, expert_gate, expert_up, expert_down):
    mixer_in = normed(hidden, mixer_gain).astype(jnp.bfloat16)
    gate_new = project(mixer_in, gate_proj).astype(jnp.bfloat16)
    value_new = project(mixer_in, value_proj).astype(jnp.bfloat16)
    write_new = project(mixer_in, write_proj).astype(jnp.bfloat16)
    read_new = project(mixer_in, read_proj).astype(jnp.bfloat16)
    step_size = jax.nn.softplus(project(mixer_in, step_proj) + step_bias)
    decay = jnp.exp(-step_size * jnp.exp(decay_log))
    value_conv = convolve(value_tail, value_new, value_taps)
    write_conv = convolve(write_tail, write_new, write_taps)
    read_conv = convolve(read_tail, read_new, read_taps)
    per_group = HEADS // BC_GROUPS
    heads_value = value_conv.reshape(TOKENS, HEADS, HEAD_DIM)
    heads_write = jnp.repeat(write_conv.reshape(TOKENS, BC_GROUPS, STATE_N), per_group, axis=1)
    heads_read = jnp.repeat(read_conv.reshape(TOKENS, BC_GROUPS, STATE_N), per_group, axis=1)
    new_state = decay[:, :, None, None] * scan_state + (step_size[:, :, None] * heads_value)[:, :, :, None] * heads_write[:, :, None, :]
    mixed_heads = jnp.einsum('thpn,thn->thp', new_state, heads_read, precision=lax.Precision.HIGHEST) + skip_gain[None, :, None] * heads_value
    gated = mixed_heads.reshape(TOKENS, DI) * jax.nn.silu(gate_new.astype(jnp.float32))
    grouped = gated.reshape(TOKENS, BC_GROUPS, DI // BC_GROUPS)
    grouped = grouped * lax.rsqrt(lax.optimization_barrier(jnp.mean(grouped * grouped, axis=-1, keepdims=True)) + EPSILON)
    mixed = (grouped.reshape(TOKENS, DI) * group_gain.astype(jnp.float32)).astype(jnp.bfloat16)
    residual = hidden.astype(jnp.float32) + project(mixed, out_proj)
    ffn_in = normed(residual, ffn_gain).astype(jnp.bfloat16)
    group_weights = jnp.exp(project(ffn_in, group_router))
    group_prob = group_weights / lax.optimization_barrier(jnp.sum(group_weights, axis=1, keepdims=True))
    group_of = (expert_choice[:, 0] // GROUP_SIZE).astype(jnp.int32)
    chosen_prob = jnp.take_along_axis(group_prob, group_of[:, None], axis=1)
    picked_exp = jnp.exp(jnp.take_along_axis(project(ffn_in, expert_router), expert_choice, axis=1))
    gates = chosen_prob * picked_exp / lax.optimization_barrier(jnp.sum(picked_exp, axis=1, keepdims=True))
    padded = jnp.concatenate([ffn_in, jnp.zeros((1, D), jnp.bfloat16)], axis=0)
    flat_choice = expert_choice.reshape(-1)
    slot_rows = N_EP * CAP
    block = EXPERT_WIDTH // N_TP

    def one_expert(expert):
        hits = jnp.nonzero(flat_choice == expert, size=slot_rows, fill_value=TOKENS * TOPK)[0].astype(jnp.int32)
        sources = jnp.minimum(hits // TOPK, TOKENS).astype(jnp.int32)
        arrived = padded[sources]
        activated = (jax.nn.silu(project(arrived, expert_gate[expert])) * project(arrived, expert_up[expert])).astype(jnp.bfloat16)
        summed = jnp.zeros((slot_rows, D), jnp.float32)
        for shard in range(N_TP):
            partial_value = project(activated[:, shard * block:(shard + 1) * block], expert_down[expert, shard * block:(shard + 1) * block]).astype(jnp.bfloat16)
            summed = summed + lax.optimization_barrier(partial_value).astype(jnp.float32)
        return (hits, summed.astype(jnp.bfloat16))
    hits, outputs = lax.map(one_expert, jnp.arange(EXPERTS, dtype=jnp.int32))
    table = jnp.zeros((TOKENS * TOPK + 1, D), jnp.bfloat16).at[hits.reshape(-1)].set(outputs.reshape(-1, D))
    expert_out = table[:TOKENS * TOPK].reshape(TOKENS, TOPK, D).astype(jnp.float32)
    layer_out = (residual + lax.optimization_barrier(jnp.sum(gates[:, :, None] * expert_out, axis=1))).astype(jnp.bfloat16)
    return (layer_out, new_state)
```

```python
import functools

import jax
import jax.numpy as jnp
from jax import lax
from jax.experimental import pallas as pl
from jax.experimental.pallas import tpu as pltpu
from jax.sharding import PartitionSpec as P

GROUP_SIZE = 8
EPSILON = 1e-06
MESH = pl.DeviceIdType.MESH
F32 = jnp.float32
BF16 = jnp.bfloat16


def dot(left, right, left_dim=1, right_dim=0, **options):
    return lax.dot_general(
        left,
        right,
        (((left_dim,), (right_dim,)), ((), ())),
        preferred_element_type=F32,
        **options,
    )


def normed(widened, gain):
    scale = lax.rsqrt(jnp.mean(widened * widened, axis=-1, keepdims=True) + EPSILON)
    return widened * scale * gain


def mixer_kernel(
    names,
    *refs,
):
    count = len(names)
    hbm = dict(zip(names, refs[:count]))
    bias_ref, rate_ref, skip_ref = refs[count : count + 3]
    mixed_ref, state_out = refs[count + 3 : count + 5]
    vmem = dict(zip(names, refs[count + 5 : 2 * count + 5]))
    y_ref, load_sem, state_sem, out_sem = refs[2 * count + 5 :]
    tp = lax.axis_index("tp")
    rows, head_count, head_dim, state_size = state_out.shape
    copies = {}
    for number, name in enumerate(names):
        if name == "state":
            for t in range(rows):
                copies["state", t] = pltpu.make_async_copy(
                    hbm[name].at[t], vmem[name].at[t], state_sem.at[t]
                )
                copies["state", t].start()
        else:
            copies[name] = pltpu.make_async_copy(hbm[name], vmem[name], load_sem.at[number])
            copies[name].start()

    def get(name):
        copies[name].wait()
        return vmem[name]

    hidden = get("hidden")[...].astype(F32)
    mixer_in = normed(hidden, get("mixer_gain")[...]).astype(BF16)
    width = vmem["value_proj"].shape[1]
    lane_head = lax.broadcasted_iota(jnp.int32, (1, width), 1) // head_dim

    def spread(ref):
        total = jnp.zeros((1, width), F32)
        for h in range(head_count):
            total = jnp.where(lane_head == h, ref[tp * head_count + h], total)
        return total

    step_raw = dot(mixer_in, get("step_proj")[...], 1, 1)
    pick = (
        lax.broadcasted_iota(jnp.int32, (step_raw.shape[1], width), 0)
        == tp * head_count + lax.broadcasted_iota(jnp.int32, (step_raw.shape[1], width), 1) // head_dim
    ).astype(F32)
    step_in = dot(step_raw, pick, precision=lax.Precision.HIGHEST) + spread(bias_ref)
    step_size = jnp.maximum(step_in, 0.0) + jnp.log1p(jnp.exp(-jnp.abs(step_in)))
    decay = jnp.exp(-step_size * jnp.exp(spread(rate_ref)))

    def convolved(kind):
        taps = get(kind + "_taps")
        tail = get(kind + "_tail")
        newest = dot(mixer_in, get(kind + "_proj")[...]).astype(BF16).astype(F32)
        span = newest.shape[1]
        kernel = taps[:, pl.ds(pl.multiple_of(tp * span, 128), span)].astype(F32)
        last = kernel.shape[0] - 1
        summed = kernel[last : last + 1] * newest
        for j in range(last):
            summed = summed + kernel[j : j + 1] * tail[j].astype(F32)
        return summed * jax.nn.sigmoid(summed)

    write_conv = convolved("write")
    read_conv = convolved("read").astype(BF16)
    value_conv = convolved("value")
    drive = (step_size * value_conv).T
    groups = write_conv.shape[1] // state_size
    per_group = head_count // groups
    group_width = per_group * head_dim
    state = vmem["state"]
    outs = []
    for t in range(rows):
        copies["state", t].wait()
        for g in range(groups):
            write_row = write_conv[t : t + 1, g * state_size : (g + 1) * state_size]
            parts = []
            for h in range(g * per_group, (g + 1) * per_group):
                updated = (
                    decay[t : t + 1, h * head_dim : h * head_dim + 1] * state[t, h]
                    + drive[h * head_dim : (h + 1) * head_dim, t : t + 1] * write_row
                )
                state[t, h] = updated
                parts.append(updated.astype(BF16))
            read_row = read_conv[t : t + 1, g * state_size : (g + 1) * state_size]
            y_ref[t : t + 1, g * group_width : (g + 1) * group_width] = dot(
                read_row, jnp.concatenate(parts, axis=0), 1, 1
            )
        out = pltpu.make_async_copy(state.at[t], state_out.at[t], out_sem.at[t])
        out.start()
        outs.append(out)
    gate_new = dot(mixer_in, get("gate_proj")[...]).astype(BF16).astype(F32)
    gated = (y_ref[...] + spread(skip_ref) * value_conv) * (gate_new * jax.nn.sigmoid(gate_new))
    gain = get("group_gain")[:, pl.ds(pl.multiple_of(tp * width, 128), width)]
    for g in range(groups):
        lanes = slice(g * group_width, (g + 1) * group_width)
        mixed_ref[:, lanes] = normed(gated[:, lanes], gain[:, lanes]).astype(BF16)
    for out in outs:
        out.wait()


def expert_kernel(
    cap,
    mixed_ref,
    hidden_ref,
    gain_ref,
    group_ref,
    router_ref,
    choice_ref,
    out_hbm,
    gate_hbm,
    up_hbm,
    down_hbm,
    result_ref,
    out_ref,
    gate_ref,
    up_ref,
    down_ref,
    part_ref,
    part_in,
    ffn_ref,
    res_ref,
    outgoing,
    arrived,
    other,
    half_out,
    half_in,
    answer,
    returned,
    load_sem,
    local_sem,
    part_sem,
    send_sem,
    recv_sem,
    relay_sem,
    landed_sem,
    half_sem,
    back_sem,
    home_sem,
):
    ep_count = lax.axis_size("ep")
    me = lax.axis_index("ep")
    tp = lax.axis_index("tp")
    barrier = pltpu.get_barrier_semaphore()
    partner = (me, 1 - tp)

    def peer(step):
        return lax.rem(me + step, ep_count)

    def source(step):
        return lax.rem(me - step + ep_count, ep_count)

    def block(number):
        return pl.ds(pl.multiple_of(number * cap, cap), cap)

    pl.semaphore_signal(barrier, inc=1, device_id=partner, device_id_type=MESH)
    for step in range(1, ep_count):
        pl.semaphore_signal(barrier, inc=1, device_id=(peer(step), tp), device_id_type=MESH)
    loads = []
    pairs = ((out_hbm, out_ref), (gate_hbm.at[0], gate_ref), (up_hbm.at[0], up_ref), (down_hbm.at[0], down_ref))
    for number, (far, near) in enumerate(pairs):
        loads.append(pltpu.make_async_copy(far, near, load_sem.at[number]))
        loads[-1].start()

    slots = arrived.shape[0]
    tokens = hidden_ref.shape[0]
    row = lax.broadcasted_iota(jnp.int32, (slots, tokens), 0)
    choice = choice_ref[...]
    hit = choice[0:1] == row // cap
    for k in range(1, choice.shape[0]):
        hit = hit | (choice[k : k + 1] == row // cap)
    hit = hit.astype(F32)
    earlier = (
        lax.broadcasted_iota(jnp.int32, (tokens, tokens), 0)
        < lax.broadcasted_iota(jnp.int32, (tokens, tokens), 1)
    ).astype(BF16)
    position = dot(hit.astype(BF16), earlier)
    dispatch = jnp.where(position == (row % cap).astype(F32), hit, 0.0)

    loads[0].wait()
    part_ref[...] = dot(mixed_ref[...], out_ref[...])
    pl.semaphore_wait(barrier, ep_count)
    swap = pltpu.make_async_remote_copy(
        part_ref, part_in, part_sem.at[0], part_sem.at[1], device_id=partner, device_id_type=MESH
    )
    swap.start()
    swap.wait()
    residual = hidden_ref[...].astype(F32) + (part_ref[...] + part_in[...])
    res_ref[...] = residual
    ffn_in = normed(residual, gain_ref[...]).astype(BF16)
    ffn_ref[...] = ffn_in.astype(F32)
    half = arrived.shape[1]
    own = pl.ds(pl.multiple_of(tp * half, 128), half)
    not_own = pl.ds(pl.multiple_of((1 - tp) * half, 128), half)
    outgoing[...] = dot(dispatch.astype(BF16), ffn_ref[:, own].astype(BF16)).astype(BF16)
    sends = []
    for step in range(1, ep_count):
        sends.append(
            pltpu.make_async_remote_copy(
                outgoing.at[block(peer(step))],
                arrived.at[block(me)],
                send_sem.at[step],
                recv_sem.at[step],
                device_id=(peer(step), tp),
                device_id_type=MESH,
            )
        )
        sends[-1].start()
    keep = pltpu.make_async_copy(outgoing.at[block(me)], arrived.at[block(me)], local_sem.at[0])
    keep.start()
    relays = [
        pltpu.make_async_remote_copy(
            outgoing.at[block(me)],
            other.at[block(me)],
            relay_sem.at[0],
            landed_sem.at[0],
            device_id=partner,
            device_id_type=MESH,
        )
    ]
    relays[0].start()

    group_exp = jnp.exp(dot(group_ref[...], ffn_in, 1, 1))
    group_prob = group_exp / jnp.sum(group_exp, axis=0, keepdims=True)
    group_row = lax.broadcasted_iota(jnp.int32, group_prob.shape, 0)
    chosen = jnp.sum(
        jnp.where(group_row == choice[0:1] // GROUP_SIZE, group_prob, 0.0), axis=0, keepdims=True
    )
    logits = dot(router_ref[...], ffn_in, 1, 1)
    experts = logits.shape[0]
    widen = (
        lax.broadcasted_iota(jnp.int32, (slots, experts), 0) // cap
        == lax.broadcasted_iota(jnp.int32, (slots, experts), 1)
    ).astype(F32)
    wide = dot(widen, logits, precision=lax.Precision.HIGHEST)
    picked = jnp.where(hit > 0.0, jnp.exp(wide), 0.0)
    total = jnp.sum(jnp.where(row % cap == 0, picked, 0.0), axis=0, keepdims=True)
    combine = (jnp.where(dispatch > 0.0, picked, 0.0) * (chosen / total)).T
    combine_high = combine.astype(BF16)
    combine_low = (combine - combine_high.astype(F32)).astype(BF16)

    for step in range(1, ep_count):
        sends[step - 1].wait_recv()
        relays.append(
            pltpu.make_async_remote_copy(
                arrived.at[block(source(step))],
                other.at[block(source(step))],
                relay_sem.at[step],
                landed_sem.at[step],
                device_id=partner,
                device_id_type=MESH,
            )
        )
        relays[-1].start()
    keep.wait()
    loads[1].wait()
    loads[2].wait()
    mine = arrived[...]
    gate_part = dot(mine, gate_ref[own, :])
    up_part = dot(mine, up_ref[own, :])
    for relay in relays:
        relay.wait_recv()
    theirs = other[...]
    gate_full = gate_part + dot(theirs, gate_ref[not_own, :])
    up_full = up_part + dot(theirs, up_ref[not_own, :])
    activated = (gate_full * jax.nn.sigmoid(gate_full) * up_full).astype(BF16)
    loads[3].wait()
    half_out[...] = dot(activated, down_ref[:, not_own]).astype(BF16)
    trade = pltpu.make_async_remote_copy(
        half_out, half_in, half_sem.at[0], half_sem.at[1], device_id=partner, device_id_type=MESH
    )
    trade.start()
    kept = dot(activated, down_ref[:, own]).astype(BF16)
    trade.wait_recv()
    answer[...] = (kept.astype(F32) + half_in[...].astype(F32)).astype(BF16)
    backs = []
    for step in range(1, ep_count):
        backs.append(
            pltpu.make_async_remote_copy(
                answer.at[block(peer(step))],
                returned.at[block(me)],
                back_sem.at[step],
                home_sem.at[step],
                device_id=(peer(step), tp),
                device_id_type=MESH,
            )
        )
        backs[-1].start()
    keep_back = pltpu.make_async_copy(answer.at[block(me)], returned.at[block(me)], local_sem.at[1])
    keep_back.start()
    trade.wait_send()
    for send in sends:
        send.wait_send()
    for relay in relays:
        relay.wait_send()
    keep_back.wait()
    for back in backs:
        back.wait_recv()
    rows_back = returned[...]
    expert_sum = dot(combine_high, rows_back) + dot(combine_low, rows_back)
    result_ref[...] = (res_ref[:, own] + expert_sum).astype(BF16)
    for back in backs:
        back.wait_send()


def on_device(
    hidden,
    mixer_gain,
    gate_proj,
    value_proj,
    write_proj,
    read_proj,
    step_proj,
    step_bias,
    decay_log,
    skip_gain,
    value_taps,
    write_taps,
    read_taps,
    value_tail,
    write_tail,
    read_tail,
    scan_state,
    group_gain,
    out_proj,
    ffn_gain,
    group_router,
    expert_router,
    expert_choice,
    expert_gate,
    expert_up,
    expert_down,
):
    ep_count = lax.axis_size("ep")
    rows, model = hidden.shape
    width = value_proj.shape[1]
    anywhere = pl.BlockSpec(memory_space=pl.ANY)
    near = pl.BlockSpec(memory_space=pltpu.VMEM)
    scalars = pl.BlockSpec(memory_space=pltpu.SMEM)
    gains = jnp.concatenate([mixer_gain, ffn_gain, group_gain]).astype(F32)
    gains = gains.reshape(1, -1)
    flip = lambda array: jnp.transpose(array, (1, 0, 2))
    operands = {
        "hidden": hidden,
        "mixer_gain": gains[:, :model],
        "step_proj": step_proj.T,
        "write_taps": write_taps,
        "write_tail": flip(write_tail),
        "write_proj": write_proj,
        "read_taps": read_taps,
        "read_tail": flip(read_tail),
        "read_proj": read_proj,
        "value_taps": value_taps,
        "value_tail": flip(value_tail),
        "value_proj": value_proj,
        "state": scan_state,
        "gate_proj": gate_proj,
        "group_gain": gains[:, 2 * model :],
    }
    names = tuple(operands)
    dma = pltpu.SemaphoreType.DMA
    mixed, new_state = pl.pallas_call(
        functools.partial(mixer_kernel, names),
        out_shape=(
            jax.ShapeDtypeStruct((rows, width), BF16),
            jax.ShapeDtypeStruct(scan_state.shape, F32),
        ),
        in_specs=[anywhere] * len(names) + [scalars] * 3,
        out_specs=(near, anywhere),
        scratch_shapes=[pltpu.VMEM(operands[name].shape, operands[name].dtype) for name in names]
        + [pltpu.VMEM((rows, width), F32), dma((len(names),)), dma((rows,)), dma((rows,))],
        name="mixer",
    )(*operands.values(), step_bias, decay_log, skip_gain)

    experts = expert_router.shape[1]
    capacity = expert_choice.shape[1] * ((rows + experts - 1) // experts)
    cap = (capacity + 7) // 8 * 8
    slots = experts * cap
    half = model // lax.axis_size("tp")
    hidden_units = expert_gate.shape[2]
    buffer = pltpu.VMEM((slots, half), BF16)
    layer_out = pl.pallas_call(
        functools.partial(expert_kernel, cap),
        out_shape=jax.ShapeDtypeStruct((rows, half), BF16),
        in_specs=[near] * 6 + [anywhere] * 4,
        out_specs=near,
        scratch_shapes=[
            pltpu.VMEM(out_proj.shape, BF16),
            pltpu.VMEM((model, hidden_units), BF16),
            pltpu.VMEM((model, hidden_units), BF16),
            pltpu.VMEM((hidden_units, model), BF16),
            pltpu.VMEM((rows, model), F32),
            pltpu.VMEM((rows, model), F32),
            pltpu.VMEM((rows, model), F32),
            pltpu.VMEM((rows, model), F32),
            buffer,
            buffer,
            buffer,
            buffer,
            buffer,
            buffer,
            buffer,
            dma((4,)),
            dma((2,)),
            dma((2,)),
            dma((ep_count,)),
            dma((ep_count,)),
            dma((ep_count,)),
            dma((ep_count,)),
            dma((2,)),
            dma((ep_count,)),
            dma((ep_count,)),
        ],
        compiler_params=pltpu.CompilerParams(collective_id=0, has_side_effects=True),
        name="experts",
    )(
        mixed,
        hidden,
        gains[:, model : 2 * model],
        group_router.T,
        expert_router.T,
        expert_choice.T,
        out_proj,
        expert_gate,
        expert_up,
        expert_down,
    )
    return (layer_out, new_state)


def solution(mesh):
    placed = (
        P("ep", None),
        P(),
        P(None, "tp"),
        P(None, "tp"),
        P(None, "tp"),
        P(None, "tp"),
        P(),
        P(),
        P(),
        P(),
        P(),
        P(),
        P(),
        P("ep", None, "tp"),
        P("ep", None, "tp"),
        P("ep", None, "tp"),
        P("ep", "tp", None, None),
        P(),
        P("tp", None),
        P(),
        P(),
        P(),
        P("ep", None),
        P("ep", None, "tp"),
        P("ep", None, "tp"),
        P("ep", "tp", None),
    )
    return jax.shard_map(
        on_device,
        mesh=mesh,
        in_specs=placed,
        out_specs=(P("ep", "tp"), P("ep", "tp", None, None)),
        check_vma=False,
    )
```

```python
import functools

import jax
import jax.numpy as jnp
from jax import lax
from jax.experimental import pallas as pl
from jax.experimental.pallas import tpu as pltpu
from jax.sharding import PartitionSpec as P

GROUP_SIZE = 8
EPSILON = 1e-06
CHUNKS = 4
MESH = pl.DeviceIdType.MESH
F32 = jnp.float32
BF16 = jnp.bfloat16


def dot(left, right, left_dim=1, right_dim=0, **options):
    return lax.dot_general(
        left,
        right,
        (((left_dim,), (right_dim,)), ((), ())),
        preferred_element_type=F32,
        **options,
    )


def row_of(ref):
    return ref[...].astype(F32).reshape(1, -1)


def normed(widened, gain):
    scale = lax.rsqrt(jnp.mean(widened * widened, axis=-1, keepdims=True) + EPSILON)
    return widened * scale * gain


def mixer_kernel(
    names,
    *refs,
):
    count = len(names)
    hbm = dict(zip(names, refs[:count]))
    bias_ref, rate_ref, skip_ref = refs[count : count + 3]
    mixed_ref, state_out = refs[count + 3 : count + 5]
    vmem = dict(zip(names, refs[count + 5 : 2 * count + 5]))
    y_ref, load_sem, state_sem, out_sem = refs[2 * count + 5 :]
    tp = lax.axis_index("tp")
    rows, head_count, head_dim, state_size = state_out.shape
    edges = [rows * c // CHUNKS for c in range(CHUNKS + 1)]
    copies = {}
    for number, name in enumerate(names):
        if name == "state":
            for c in range(CHUNKS):
                span = pl.ds(edges[c], edges[c + 1] - edges[c])
                copies["state", c] = pltpu.make_async_copy(
                    hbm[name].at[span], vmem[name].at[span], state_sem.at[c]
                )
                copies["state", c].start()
        else:
            copies[name] = pltpu.make_async_copy(hbm[name], vmem[name], load_sem.at[number])
            copies[name].start()

    def get(name):
        copies[name].wait()
        return vmem[name]

    hidden = get("hidden")[...].astype(F32)
    mixer_in = normed(hidden, row_of(get("mixer_gain"))).astype(BF16)
    width = vmem["value_proj"].shape[1]
    lane_head = lax.broadcasted_iota(jnp.int32, (1, width), 1) // head_dim

    def spread(ref):
        total = jnp.zeros((1, width), F32)
        for h in range(head_count):
            total = jnp.where(lane_head == h, ref[tp * head_count + h], total)
        return total

    step_raw = dot(mixer_in, get("step_proj")[...], 1, 1)
    pick = (
        lax.broadcasted_iota(jnp.int32, (step_raw.shape[1], width), 0)
        == tp * head_count + lax.broadcasted_iota(jnp.int32, (step_raw.shape[1], width), 1) // head_dim
    ).astype(F32)
    step_in = dot(step_raw, pick, precision=lax.Precision.HIGHEST) + spread(bias_ref)
    step_size = jnp.maximum(step_in, 0.0) + jnp.log1p(jnp.exp(-jnp.abs(step_in)))
    decay = jnp.exp(-step_size * jnp.exp(spread(rate_ref)))

    def convolved(kind):
        taps = get(kind + "_taps")
        tail = get(kind + "_tail")
        newest = dot(mixer_in, get(kind + "_proj")[...]).astype(BF16).astype(F32)
        span = newest.shape[1]
        kernel = taps[:, pl.ds(pl.multiple_of(tp * span, 128), span)].astype(F32)
        last = kernel.shape[0] - 1
        summed = kernel[last : last + 1] * newest
        for j in range(last):
            summed = summed + kernel[j : j + 1] * tail[j].astype(F32)
        return summed * jax.nn.sigmoid(summed)

    write_conv = convolved("write")
    read_conv = convolved("read").astype(BF16)
    value_conv = convolved("value")
    drive = (step_size * value_conv).T
    groups = write_conv.shape[1] // state_size
    per_group = head_count // groups
    group_width = per_group * head_dim
    state = vmem["state"]
    outs = []
    def token(t):
        for g in range(groups):
            write_row = write_conv[t : t + 1, g * state_size : (g + 1) * state_size]
            parts = []
            for h in range(g * per_group, (g + 1) * per_group):
                updated = (
                    decay[t : t + 1, h * head_dim : h * head_dim + 1] * state[t, h]
                    + drive[h * head_dim : (h + 1) * head_dim, t : t + 1] * write_row
                )
                state[t, h] = updated
                parts.append(updated.astype(BF16))
            read_row = read_conv[t : t + 1, g * state_size : (g + 1) * state_size]
            y_ref[t : t + 1, g * group_width : (g + 1) * group_width] = dot(
                read_row, jnp.concatenate(parts, axis=0), 1, 1
            )

    gate_new = dot(mixer_in, get("gate_proj")[...]).astype(BF16).astype(F32)
    gate_new = gate_new * jax.nn.sigmoid(gate_new)
    gain = get("group_gain")
    for c in range(CHUNKS):
        copies["state", c].wait()
        for t in range(edges[c], edges[c + 1]):
            token(t)
        span = pl.ds(edges[c], edges[c + 1] - edges[c])
        outs.append(pltpu.make_async_copy(state.at[span], state_out.at[span], out_sem.at[c]))
        outs[-1].start()
    gain_row = gain[pl.ds(pl.multiple_of(tp * width, width), width)].astype(F32).reshape(1, width)
    gated = (y_ref[...] + spread(skip_ref) * value_conv) * gate_new
    for g in range(groups):
        lanes = slice(g * group_width, (g + 1) * group_width)
        mixed_ref[:, lanes] = normed(gated[:, lanes], gain_row[:, lanes]).astype(BF16)
    for out in outs:
        out.wait()


def expert_kernel(
    cap,
    mixed_ref,
    hidden_ref,
    gain_ref,
    group_ref,
    router_ref,
    choice_ref,
    out_hbm,
    gate_hbm,
    up_hbm,
    down_hbm,
    result_ref,
    out_ref,
    gate_ref,
    up_ref,
    down_ref,
    part_ref,
    part_in,
    ffn_ref,
    res_ref,
    outgoing,
    arrived,
    other,
    half_out,
    half_in,
    answer,
    returned,
    load_sem,
    local_sem,
    part_sem,
    send_sem,
    recv_sem,
    relay_sem,
    landed_sem,
    half_sem,
    back_sem,
    home_sem,
):
    ep_count = lax.axis_size("ep")
    me = lax.axis_index("ep")
    tp = lax.axis_index("tp")
    barrier = pltpu.get_barrier_semaphore()
    partner = (me, 1 - tp)

    def peer(step):
        return lax.rem(me + step, ep_count)

    def source(step):
        return lax.rem(me - step + ep_count, ep_count)

    def block(number):
        return pl.ds(pl.multiple_of(number * cap, cap), cap)

    pl.semaphore_signal(barrier, inc=1, device_id=partner, device_id_type=MESH)
    for step in range(1, ep_count):
        pl.semaphore_signal(barrier, inc=1, device_id=(peer(step), tp), device_id_type=MESH)
    loads = []
    pairs = ((out_hbm, out_ref), (gate_hbm.at[0], gate_ref), (up_hbm.at[0], up_ref), (down_hbm.at[0], down_ref))
    for number, (far, near) in enumerate(pairs):
        loads.append(pltpu.make_async_copy(far, near, load_sem.at[number]))
        loads[-1].start()

    slots = arrived.shape[0]
    tokens = hidden_ref.shape[0]
    row = lax.broadcasted_iota(jnp.int32, (slots, tokens), 0)
    choice = choice_ref[...]
    hit = choice[0:1] == row // cap
    for k in range(1, choice.shape[0]):
        hit = hit | (choice[k : k + 1] == row // cap)
    hit = hit.astype(F32)
    earlier = (
        lax.broadcasted_iota(jnp.int32, (tokens, tokens), 0)
        < lax.broadcasted_iota(jnp.int32, (tokens, tokens), 1)
    ).astype(BF16)
    position = dot(hit.astype(BF16), earlier)
    dispatch = jnp.where(position == (row % cap).astype(F32), hit, 0.0)

    loads[0].wait()
    part_ref[...] = dot(mixed_ref[...], out_ref[...])
    pl.semaphore_wait(barrier, ep_count)
    swap = pltpu.make_async_remote_copy(
        part_ref, part_in, part_sem.at[0], part_sem.at[1], device_id=partner, device_id_type=MESH
    )
    swap.start()
    swap.wait()
    residual = hidden_ref[...].astype(F32) + (part_ref[...] + part_in[...])
    res_ref[...] = residual
    ffn_in = normed(residual, row_of(gain_ref)).astype(BF16)
    ffn_ref[...] = ffn_in.astype(F32)
    half = arrived.shape[1]
    own = pl.ds(pl.multiple_of(tp * half, 128), half)
    not_own = pl.ds(pl.multiple_of((1 - tp) * half, 128), half)
    outgoing[...] = dot(dispatch.astype(BF16), ffn_ref[:, own].astype(BF16)).astype(BF16)
    sends = {}
    steps = sorted(range(1, ep_count), key=lambda step: abs(2 * step - ep_count))
    for step in steps:
        sends[step] = (
            pltpu.make_async_remote_copy(
                outgoing.at[block(peer(step))],
                arrived.at[block(me)],
                send_sem.at[step],
                recv_sem.at[step],
                device_id=(peer(step), tp),
                device_id_type=MESH,
            )
        )
        sends[step].start()
    keep = pltpu.make_async_copy(outgoing.at[block(me)], arrived.at[block(me)], local_sem.at[0])
    keep.start()
    relays = [
        pltpu.make_async_remote_copy(
            outgoing.at[block(me)],
            other.at[block(me)],
            relay_sem.at[0],
            landed_sem.at[0],
            device_id=partner,
            device_id_type=MESH,
        )
    ]
    relays[0].start()

    group_exp = jnp.exp(dot(group_ref[...], ffn_in, 1, 1))
    group_prob = group_exp / jnp.sum(group_exp, axis=0, keepdims=True)
    group_row = lax.broadcasted_iota(jnp.int32, group_prob.shape, 0)
    chosen = jnp.sum(
        jnp.where(group_row == choice[0:1] // GROUP_SIZE, group_prob, 0.0), axis=0, keepdims=True
    )
    logits = dot(router_ref[...], ffn_in, 1, 1)
    experts = logits.shape[0]
    widen = (
        lax.broadcasted_iota(jnp.int32, (slots, experts), 0) // cap
        == lax.broadcasted_iota(jnp.int32, (slots, experts), 1)
    ).astype(F32)
    wide = dot(widen, logits, precision=lax.Precision.HIGHEST)
    picked = jnp.where(hit > 0.0, jnp.exp(wide), 0.0)
    total = jnp.sum(jnp.where(row % cap == 0, picked, 0.0), axis=0, keepdims=True)
    combine = (jnp.where(dispatch > 0.0, picked, 0.0) * (chosen / total)).T
    combine_high = combine.astype(BF16)
    combine_low = (combine - combine_high.astype(F32)).astype(BF16)

    for step in reversed(steps):
        sends[step].wait_recv()
        relays.append(
            pltpu.make_async_remote_copy(
                arrived.at[block(source(step))],
                other.at[block(source(step))],
                relay_sem.at[step],
                landed_sem.at[step],
                device_id=partner,
                device_id_type=MESH,
            )
        )
        relays[-1].start()
    keep.wait()
    loads[1].wait()
    loads[2].wait()
    mine = arrived[...]
    gate_part = dot(mine, gate_ref[own, :])
    up_part = dot(mine, up_ref[own, :])
    for relay in relays:
        relay.wait_recv()
    theirs = other[...]
    gate_full = gate_part + dot(theirs, gate_ref[not_own, :])
    up_full = up_part + dot(theirs, up_ref[not_own, :])
    activated = (gate_full * jax.nn.sigmoid(gate_full) * up_full).astype(BF16)
    loads[3].wait()
    half_out[...] = dot(activated, down_ref[:, not_own]).astype(BF16)
    trade = pltpu.make_async_remote_copy(
        half_out, half_in, half_sem.at[0], half_sem.at[1], device_id=partner, device_id_type=MESH
    )
    trade.start()
    kept = dot(activated, down_ref[:, own]).astype(BF16)
    trade.wait_recv()
    answer[...] = (kept.astype(F32) + half_in[...].astype(F32)).astype(BF16)
    backs = []
    for step in steps:
        backs.append(
            pltpu.make_async_remote_copy(
                answer.at[block(peer(step))],
                returned.at[block(me)],
                back_sem.at[step],
                home_sem.at[step],
                device_id=(peer(step), tp),
                device_id_type=MESH,
            )
        )
        backs[-1].start()
    keep_back = pltpu.make_async_copy(answer.at[block(me)], returned.at[block(me)], local_sem.at[1])
    keep_back.start()
    trade.wait_send()
    for send in sends.values():
        send.wait_send()
    for relay in relays:
        relay.wait_send()
    keep_back.wait()
    for back in backs:
        back.wait_recv()
    rows_back = returned[...]
    expert_sum = dot(combine_high, rows_back) + dot(combine_low, rows_back)
    result_ref[...] = (res_ref[:, own] + expert_sum).astype(BF16)
    for back in backs:
        back.wait_send()


def on_device(
    hidden,
    mixer_gain,
    gate_proj,
    value_proj,
    write_proj,
    read_proj,
    step_proj,
    step_bias,
    decay_log,
    skip_gain,
    value_taps,
    write_taps,
    read_taps,
    value_tail,
    write_tail,
    read_tail,
    scan_state,
    group_gain,
    out_proj,
    ffn_gain,
    group_router,
    expert_router,
    expert_choice,
    expert_gate,
    expert_up,
    expert_down,
):
    ep_count = lax.axis_size("ep")
    rows, model = hidden.shape
    width = value_proj.shape[1]
    anywhere = pl.BlockSpec(memory_space=pl.ANY)
    near = pl.BlockSpec(memory_space=pltpu.VMEM)
    scalars = pl.BlockSpec(memory_space=pltpu.SMEM)
    flip = lambda array: jnp.transpose(array, (1, 0, 2))
    operands = {
        "hidden": hidden,
        "mixer_gain": mixer_gain,
        "step_proj": step_proj.T,
        "write_taps": write_taps,
        "write_tail": flip(write_tail),
        "write_proj": write_proj,
        "read_taps": read_taps,
        "read_tail": flip(read_tail),
        "read_proj": read_proj,
        "value_taps": value_taps,
        "value_tail": flip(value_tail),
        "value_proj": value_proj,
        "gate_proj": gate_proj,
        "state": scan_state,
        "group_gain": group_gain,
    }
    names = tuple(operands)
    dma = pltpu.SemaphoreType.DMA
    mixed, new_state = pl.pallas_call(
        functools.partial(mixer_kernel, names),
        out_shape=(
            jax.ShapeDtypeStruct((rows, width), BF16),
            jax.ShapeDtypeStruct(scan_state.shape, F32),
        ),
        in_specs=[anywhere] * len(names) + [scalars] * 3,
        out_specs=(near, anywhere),
        scratch_shapes=[pltpu.VMEM(operands[name].shape, operands[name].dtype) for name in names]
        + [pltpu.VMEM((rows, width), F32), dma((len(names),)), dma((CHUNKS,)), dma((CHUNKS,))],
        name="mixer",
    )(*operands.values(), step_bias, decay_log, skip_gain)

    experts = expert_router.shape[1]
    capacity = expert_choice.shape[1] * ((rows + experts - 1) // experts)
    cap = (capacity + 7) // 8 * 8
    slots = experts * cap
    half = model // lax.axis_size("tp")
    hidden_units = expert_gate.shape[2]
    buffer = pltpu.VMEM((slots, half), BF16)
    layer_out = pl.pallas_call(
        functools.partial(expert_kernel, cap),
        out_shape=jax.ShapeDtypeStruct((rows, half), BF16),
        in_specs=[near] * 6 + [anywhere] * 4,
        out_specs=near,
        scratch_shapes=[
            pltpu.VMEM(out_proj.shape, BF16),
            pltpu.VMEM((model, hidden_units), BF16),
            pltpu.VMEM((model, hidden_units), BF16),
            pltpu.VMEM((hidden_units, model), BF16),
            pltpu.VMEM((rows, model), F32),
            pltpu.VMEM((rows, model), F32),
            pltpu.VMEM((rows, model), F32),
            pltpu.VMEM((rows, model), F32),
            buffer,
            buffer,
            buffer,
            buffer,
            buffer,
            buffer,
            buffer,
            dma((4,)),
            dma((2,)),
            dma((2,)),
            dma((ep_count,)),
            dma((ep_count,)),
            dma((ep_count,)),
            dma((ep_count,)),
            dma((2,)),
            dma((ep_count,)),
            dma((ep_count,)),
        ],
        compiler_params=pltpu.CompilerParams(collective_id=0, has_side_effects=True),
        name="experts",
    )(
        mixed,
        hidden,
        ffn_gain,
        group_router.T,
        expert_router.T,
        expert_choice.T,
        out_proj,
        expert_gate,
        expert_up,
        expert_down,
    )
    return (layer_out, new_state)


def solution(mesh):
    placed = (
        P("ep", None),
        P(),
        P(None, "tp"),
        P(None, "tp"),
        P(None, "tp"),
        P(None, "tp"),
        P(),
        P(),
        P(),
        P(),
        P(),
        P(),
        P(),
        P("ep", None, "tp"),
        P("ep", None, "tp"),
        P("ep", None, "tp"),
        P("ep", "tp", None, None),
        P(),
        P("tp", None),
        P(),
        P(),
        P(),
        P("ep", None),
        P("ep", None, "tp"),
        P("ep", None, "tp"),
        P("ep", "tp", None),
    )
    return jax.shard_map(
        on_device,
        mesh=mesh,
        in_specs=placed,
        out_specs=(P("ep", "tp"), P("ep", "tp", None, None)),
        check_vma=False,
    )
```

```python
import functools

import jax
import jax.numpy as jnp
from jax import lax
from jax.experimental import pallas as pl
from jax.experimental.pallas import tpu as pltpu
from jax.sharding import PartitionSpec as P

GROUP_SIZE = 8
EPSILON = 1e-06
CHUNKS = 4
MESH = pl.DeviceIdType.MESH
F32 = jnp.float32
BF16 = jnp.bfloat16


def dot(left, right, left_dim=1, right_dim=0, **options):
    return lax.dot_general(
        left,
        right,
        (((left_dim,), (right_dim,)), ((), ())),
        preferred_element_type=F32,
        **options,
    )


def row_of(ref):
    return ref[...].astype(F32).reshape(1, -1)


def normed(widened, gain):
    scale = lax.rsqrt(jnp.mean(widened * widened, axis=-1, keepdims=True) + EPSILON)
    return widened * scale * gain


def mixer_kernel(
    names,
    *refs,
):
    count = len(names)
    hbm = dict(zip(names, refs[:count]))
    bias_ref, rate_ref, skip_ref = refs[count : count + 3]
    mixed_ref, state_out = refs[count + 3 : count + 5]
    vmem = dict(zip(names, refs[count + 5 : 2 * count + 5]))
    y_ref, load_sem, state_sem, out_sem = refs[2 * count + 5 :]
    tp = lax.axis_index("tp")
    rows, head_count, head_dim, state_size = state_out.shape
    edges = [rows * c // CHUNKS for c in range(CHUNKS + 1)]
    copies = {}
    for number, name in enumerate(names):
        if name == "state":
            for c in range(CHUNKS):
                span = pl.ds(edges[c], edges[c + 1] - edges[c])
                copies["state", c] = pltpu.make_async_copy(
                    hbm[name].at[span], vmem[name].at[span], state_sem.at[c]
                )
                copies["state", c].start()
        else:
            copies[name] = pltpu.make_async_copy(hbm[name], vmem[name], load_sem.at[number])
            copies[name].start()

    def get(name):
        copies[name].wait()
        return vmem[name]

    hidden = get("hidden")[...].astype(F32)
    mixer_in = normed(hidden, row_of(get("mixer_gain"))).astype(BF16)
    width = vmem["value_proj"].shape[1]
    lane_head = lax.broadcasted_iota(jnp.int32, (1, width), 1) // head_dim

    def spread(ref):
        total = jnp.zeros((1, width), F32)
        for h in range(head_count):
            total = jnp.where(lane_head == h, ref[tp * head_count + h], total)
        return total

    step_raw = dot(mixer_in, get("step_proj")[...], 1, 1)
    pick = (
        lax.broadcasted_iota(jnp.int32, (step_raw.shape[1], width), 0)
        == tp * head_count + lax.broadcasted_iota(jnp.int32, (step_raw.shape[1], width), 1) // head_dim
    ).astype(F32)
    step_in = dot(step_raw, pick, precision=lax.Precision.HIGHEST) + spread(bias_ref)
    step_size = jnp.maximum(step_in, 0.0) + jnp.log1p(jnp.exp(-jnp.abs(step_in)))
    decay = jnp.exp(-step_size * jnp.exp(spread(rate_ref)))

    def convolved(kind):
        taps = get(kind + "_taps")
        tail = get(kind + "_tail")
        newest = dot(mixer_in, get(kind + "_proj")[...]).astype(BF16).astype(F32)
        span = newest.shape[1]
        kernel = taps[:, pl.ds(pl.multiple_of(tp * span, 128), span)].astype(F32)
        last = kernel.shape[0] - 1
        summed = kernel[last : last + 1] * newest
        for j in range(last):
            summed = summed + kernel[j : j + 1] * tail[j].astype(F32)
        return summed * jax.nn.sigmoid(summed)

    write_conv = convolved("write")
    read_conv = convolved("read").astype(BF16)
    value_conv = convolved("value")
    drive = (step_size * value_conv).T
    groups = write_conv.shape[1] // state_size
    per_group = head_count // groups
    group_width = per_group * head_dim
    state = vmem["state"]
    outs = []
    def token(t):
        for g in range(groups):
            write_row = write_conv[t : t + 1, g * state_size : (g + 1) * state_size]
            parts = []
            for h in range(g * per_group, (g + 1) * per_group):
                updated = (
                    decay[t : t + 1, h * head_dim : h * head_dim + 1] * state[t, h]
                    + drive[h * head_dim : (h + 1) * head_dim, t : t + 1] * write_row
                )
                state[t, h] = updated
                parts.append(updated.astype(BF16))
            read_row = read_conv[t : t + 1, g * state_size : (g + 1) * state_size]
            y_ref[t : t + 1, g * group_width : (g + 1) * group_width] = dot(
                read_row, jnp.concatenate(parts, axis=0), 1, 1
            )

    gate_new = dot(mixer_in, get("gate_proj")[...]).astype(BF16).astype(F32)
    gate_new = gate_new * jax.nn.sigmoid(gate_new)
    gain = get("group_gain")
    for c in range(CHUNKS):
        copies["state", c].wait()
        for t in range(edges[c], edges[c + 1]):
            token(t)
        span = pl.ds(edges[c], edges[c + 1] - edges[c])
        outs.append(pltpu.make_async_copy(state.at[span], state_out.at[span], out_sem.at[c]))
        outs[-1].start()
    gain_row = gain[pl.ds(pl.multiple_of(tp * width, width), width)].astype(F32).reshape(1, width)
    gated = (y_ref[...] + spread(skip_ref) * value_conv) * gate_new
    for g in range(groups):
        lanes = slice(g * group_width, (g + 1) * group_width)
        mixed_ref[:, lanes] = normed(gated[:, lanes], gain_row[:, lanes]).astype(BF16)
    for out in outs:
        out.wait()


def expert_kernel(
    cap,
    mixed_ref,
    hidden_ref,
    gain_ref,
    group_ref,
    router_ref,
    choice_ref,
    out_hbm,
    gate_hbm,
    up_hbm,
    down_hbm,
    result_ref,
    out_ref,
    gate_ref,
    up_ref,
    down_ref,
    part_ref,
    part_in,
    ffn_ref,
    res_ref,
    outgoing,
    arrived,
    other,
    half_out,
    half_in,
    answer,
    returned,
    load_sem,
    local_sem,
    part_sem,
    send_sem,
    recv_sem,
    relay_sem,
    landed_sem,
    half_sem,
    back_sem,
    home_sem,
):
    ep_count = lax.axis_size("ep")
    me = lax.axis_index("ep")
    tp = lax.axis_index("tp")
    barrier = pltpu.get_barrier_semaphore()
    partner = (me, 1 - tp)

    def peer(step):
        return lax.rem(me + step, ep_count)

    def source(step):
        return lax.rem(me - step + ep_count, ep_count)

    def block(number):
        return pl.ds(pl.multiple_of(number * cap, cap), cap)

    pl.semaphore_signal(barrier, inc=1, device_id=partner, device_id_type=MESH)
    for step in range(1, ep_count):
        pl.semaphore_signal(barrier, inc=1, device_id=(peer(step), tp), device_id_type=MESH)
    loads = []
    pairs = ((out_hbm, out_ref), (gate_hbm.at[0], gate_ref), (up_hbm.at[0], up_ref), (down_hbm.at[0], down_ref))
    for number, (far, near) in enumerate(pairs):
        loads.append(pltpu.make_async_copy(far, near, load_sem.at[number]))
        loads[-1].start()

    slots = arrived.shape[0]
    tokens = hidden_ref.shape[0]
    row = lax.broadcasted_iota(jnp.int32, (slots, tokens), 0)
    choice = choice_ref[...]
    hit = choice[0:1] == row // cap
    for k in range(1, choice.shape[0]):
        hit = hit | (choice[k : k + 1] == row // cap)
    hit = hit.astype(F32)
    earlier = (
        lax.broadcasted_iota(jnp.int32, (tokens, tokens), 0)
        < lax.broadcasted_iota(jnp.int32, (tokens, tokens), 1)
    ).astype(BF16)
    position = dot(hit.astype(BF16), earlier)
    dispatch = jnp.where(position == (row % cap).astype(F32), hit, 0.0)

    loads[0].wait()
    part_ref[...] = dot(mixed_ref[...], out_ref[...])
    pl.semaphore_wait(barrier, ep_count)
    swap = pltpu.make_async_remote_copy(
        part_ref, part_in, part_sem.at[0], part_sem.at[1], device_id=partner, device_id_type=MESH
    )
    swap.start()
    swap.wait()
    residual = hidden_ref[...].astype(F32) + (part_ref[...] + part_in[...])
    res_ref[...] = residual
    ffn_in = normed(residual, row_of(gain_ref)).astype(BF16)
    ffn_ref[...] = ffn_in.astype(F32)
    half = arrived.shape[1]
    own = pl.ds(pl.multiple_of(tp * half, 128), half)
    not_own = pl.ds(pl.multiple_of((1 - tp) * half, 128), half)
    outgoing[...] = dot(dispatch.astype(BF16), ffn_ref[:, own].astype(BF16)).astype(BF16)
    sends = {}
    steps = range(1, ep_count)
    for step in steps:
        sends[step] = (
            pltpu.make_async_remote_copy(
                outgoing.at[block(peer(step))],
                arrived.at[block(me)],
                send_sem.at[step],
                recv_sem.at[step],
                device_id=(peer(step), tp),
                device_id_type=MESH,
            )
        )
        sends[step].start()
    keep = pltpu.make_async_copy(outgoing.at[block(me)], arrived.at[block(me)], local_sem.at[0])
    keep.start()
    relays = [
        pltpu.make_async_remote_copy(
            outgoing.at[block(me)],
            other.at[block(me)],
            relay_sem.at[0],
            landed_sem.at[0],
            device_id=partner,
            device_id_type=MESH,
        )
    ]
    relays[0].start()

    group_exp = jnp.exp(dot(group_ref[...], ffn_in, 1, 1))
    group_prob = group_exp / jnp.sum(group_exp, axis=0, keepdims=True)
    group_row = lax.broadcasted_iota(jnp.int32, group_prob.shape, 0)
    chosen = jnp.sum(
        jnp.where(group_row == choice[0:1] // GROUP_SIZE, group_prob, 0.0), axis=0, keepdims=True
    )
    logits = dot(router_ref[...], ffn_in, 1, 1)
    experts = logits.shape[0]
    widen = (
        lax.broadcasted_iota(jnp.int32, (slots, experts), 0) // cap
        == lax.broadcasted_iota(jnp.int32, (slots, experts), 1)
    ).astype(F32)
    wide = dot(widen, logits, precision=lax.Precision.HIGHEST)
    picked = jnp.where(hit > 0.0, jnp.exp(wide), 0.0)
    total = jnp.sum(jnp.where(row % cap == 0, picked, 0.0), axis=0, keepdims=True)
    combine = (jnp.where(dispatch > 0.0, picked, 0.0) * (chosen / total)).T
    combine_high = combine.astype(BF16)
    combine_low = (combine - combine_high.astype(F32)).astype(BF16)

    for step in steps:
        sends[step].wait_recv()
        relays.append(
            pltpu.make_async_remote_copy(
                arrived.at[block(source(step))],
                other.at[block(source(step))],
                relay_sem.at[step],
                landed_sem.at[step],
                device_id=partner,
                device_id_type=MESH,
            )
        )
        relays[-1].start()
    keep.wait()
    loads[1].wait()
    loads[2].wait()
    mine = arrived[...]
    gate_part = dot(mine, gate_ref[own, :])
    up_part = dot(mine, up_ref[own, :])
    for relay in relays:
        relay.wait_recv()
    theirs = other[...]
    gate_full = gate_part + dot(theirs, gate_ref[not_own, :])
    up_full = up_part + dot(theirs, up_ref[not_own, :])
    activated = (gate_full * jax.nn.sigmoid(gate_full) * up_full).astype(BF16)
    loads[3].wait()
    half_out[...] = dot(activated, down_ref[:, not_own]).astype(BF16)
    trade = pltpu.make_async_remote_copy(
        half_out, half_in, half_sem.at[0], half_sem.at[1], device_id=partner, device_id_type=MESH
    )
    trade.start()
    kept = dot(activated, down_ref[:, own]).astype(BF16)
    trade.wait_recv()
    answer[...] = (kept.astype(F32) + half_in[...].astype(F32)).astype(BF16)
    backs = []
    for step in steps:
        backs.append(
            pltpu.make_async_remote_copy(
                answer.at[block(peer(step))],
                returned.at[block(me)],
                back_sem.at[step],
                home_sem.at[step],
                device_id=(peer(step), tp),
                device_id_type=MESH,
            )
        )
        backs[-1].start()
    keep_back = pltpu.make_async_copy(answer.at[block(me)], returned.at[block(me)], local_sem.at[1])
    keep_back.start()
    trade.wait_send()
    for send in sends.values():
        send.wait_send()
    for relay in relays:
        relay.wait_send()
    keep_back.wait()
    for back in backs:
        back.wait_recv()
    rows_back = returned[...]
    expert_sum = dot(combine_high, rows_back) + dot(combine_low, rows_back)
    result_ref[...] = (res_ref[:, own] + expert_sum).astype(BF16)
    for back in backs:
        back.wait_send()


def on_device(
    hidden,
    mixer_gain,
    gate_proj,
    value_proj,
    write_proj,
    read_proj,
    step_proj,
    step_bias,
    decay_log,
    skip_gain,
    value_taps,
    write_taps,
    read_taps,
    value_tail,
    write_tail,
    read_tail,
    scan_state,
    group_gain,
    out_proj,
    ffn_gain,
    group_router,
    expert_router,
    expert_choice,
    expert_gate,
    expert_up,
    expert_down,
):
    ep_count = lax.axis_size("ep")
    rows, model = hidden.shape
    width = value_proj.shape[1]
    anywhere = pl.BlockSpec(memory_space=pl.ANY)
    near = pl.BlockSpec(memory_space=pltpu.VMEM)
    scalars = pl.BlockSpec(memory_space=pltpu.SMEM)
    flip = lambda array: jnp.transpose(array, (1, 0, 2))
    operands = {
        "hidden": hidden,
        "mixer_gain": mixer_gain,
        "step_proj": step_proj.T,
        "write_taps": write_taps,
        "write_tail": flip(write_tail),
        "write_proj": write_proj,
        "read_taps": read_taps,
        "read_tail": flip(read_tail),
        "read_proj": read_proj,
        "value_taps": value_taps,
        "value_tail": flip(value_tail),
        "value_proj": value_proj,
        "gate_proj": gate_proj,
        "state": scan_state,
        "group_gain": group_gain,
    }
    names = tuple(operands)
    dma = pltpu.SemaphoreType.DMA
    mixed, new_state = pl.pallas_call(
        functools.partial(mixer_kernel, names),
        out_shape=(
            jax.ShapeDtypeStruct((rows, width), BF16),
            jax.ShapeDtypeStruct(scan_state.shape, F32),
        ),
        in_specs=[anywhere] * len(names) + [scalars] * 3,
        out_specs=(near, anywhere),
        scratch_shapes=[pltpu.VMEM(operands[name].shape, operands[name].dtype) for name in names]
        + [pltpu.VMEM((rows, width), F32), dma((len(names),)), dma((CHUNKS,)), dma((CHUNKS,))],
        name="mixer",
    )(*operands.values(), step_bias, decay_log, skip_gain)

    experts = expert_router.shape[1]
    capacity = expert_choice.shape[1] * ((rows + experts - 1) // experts)
    cap = (capacity + 7) // 8 * 8
    slots = experts * cap
    half = model // lax.axis_size("tp")
    hidden_units = expert_gate.shape[2]
    buffer = pltpu.VMEM((slots, half), BF16)
    layer_out = pl.pallas_call(
        functools.partial(expert_kernel, cap),
        out_shape=jax.ShapeDtypeStruct((rows, half), BF16),
        in_specs=[near] * 6 + [anywhere] * 4,
        out_specs=near,
        scratch_shapes=[
            pltpu.VMEM(out_proj.shape, BF16),
            pltpu.VMEM((model, hidden_units), BF16),
            pltpu.VMEM((model, hidden_units), BF16),
            pltpu.VMEM((hidden_units, model), BF16),
            pltpu.VMEM((rows, model), F32),
            pltpu.VMEM((rows, model), F32),
            pltpu.VMEM((rows, model), F32),
            pltpu.VMEM((rows, model), F32),
            buffer,
            buffer,
            buffer,
            buffer,
            buffer,
            buffer,
            buffer,
            dma((4,)),
            dma((2,)),
            dma((2,)),
            dma((ep_count,)),
            dma((ep_count,)),
            dma((ep_count,)),
            dma((ep_count,)),
            dma((2,)),
            dma((ep_count,)),
            dma((ep_count,)),
        ],
        compiler_params=pltpu.CompilerParams(collective_id=0, has_side_effects=True),
        name="experts",
    )(
        mixed,
        hidden,
        ffn_gain,
        group_router.T,
        expert_router.T,
        expert_choice.T,
        out_proj,
        expert_gate,
        expert_up,
        expert_down,
    )
    return (layer_out, new_state)


def solution(mesh):
    placed = (
        P("ep", None),
        P(),
        P(None, "tp"),
        P(None, "tp"),
        P(None, "tp"),
        P(None, "tp"),
        P(),
        P(),
        P(),
        P(),
        P(),
        P(),
        P(),
        P("ep", None, "tp"),
        P("ep", None, "tp"),
        P("ep", None, "tp"),
        P("ep", "tp", None, None),
        P(),
        P("tp", None),
        P(),
        P(),
        P(),
        P("ep", None),
        P("ep", None, "tp"),
        P("ep", None, "tp"),
        P("ep", "tp", None),
    )
    return jax.shard_map(
        on_device,
        mesh=mesh,
        in_specs=placed,
        out_specs=(P("ep", "tp"), P("ep", "tp", None, None)),
        check_vma=False,
    )
```
